32 devices in a mesh: sp: 4 (over z), tp: 4 (over y, x), dp: 2 (over core).
Axes of the slice: x: 2, y: 2, z: 4, core: 2. Of those that a mesh axis runs over, the one named last changes fastest.
Arguments:
- latent: bfloat16 [2, 768, 2048], P('dp', 'sp'), may hold values from -6 to 6
- cond: bfloat16 [2, 2048], P('dp', 'sp'), may hold values from -6 to 6
- context: bfloat16 [2, 32, 2048], P('dp', 'sp'), may hold values from -6 to 6
- ctx_cond: bfloat16 [2048], P('sp'), may hold values from -6 to 6
- w_mod: bfloat16 [2048, 6144], P('sp', 'tp'), may hold values from -0.125 to 0.125
- norm_gain: bfloat16 [2048], replicated, may hold values from 0.099609375 to 1.8984375
- w_query: bfloat16 [2048, 1024], P(None, 'tp'), may hold values from -0.125 to 0.125
- w_key: bfloat16 [2048, 1024], P(None, 'tp'), may hold values from -0.125 to 0.125
- w_value: bfloat16 [2048, 1024], P(None, 'tp'), may hold values from -0.125 to 0.125
- w_outgate: bfloat16 [2048, 1024], P(None, 'tp'), may hold values from -0.125 to 0.125
- w_decay: bfloat16 [2048, 2, 8], P(None, None, 'tp'), may hold values from -0.125 to 0.125
- w_beta: bfloat16 [2048, 2, 8], P(None, None, 'tp'), may hold values from -0.125 to 0.125
- decay_rate: float32 [2, 8], P(None, 'tp'), may hold values from 6.510417e-05 to 0.0333333333
- decay_bias: float32 [2, 8], P(None, 'tp'), may hold values from -3 to 3
- extra_decay: float32 [2, 2, 8, 768], P('dp', None, 'tp', 'sp'), may hold values from -0.7007812 to -0.000130208333
- out_gain: bfloat16 [128], replicated, may hold values from 0.099609375 to 1.8984375
- w_out: bfloat16 [1024, 2048], replicated, may hold values from -0.1875 to 0.1875
Outputs:
- mixed_out: bfloat16 [2, 768, 2048], P('dp', ('sp', 'tp'))
The draws below stay inside these ranges and needn't reach their ends.
All inputs are finite; a program needn't handle non-finite values.
Results may differ from the reference program's by a relative error of at most 0.0067.
Values may be sent and summed in bfloat16 or wider, within the bound.
A program may use at most 128 MiB of HBM per device.

```python
import math
import jax
import jax.numpy as jnp
from jax import lax

D = 2048
HEADS = 8
HEAD = 128
BLOCK = 64
TOK_DEV = 192
SAMPLES = 2
LATENT_TOKENS = 768
CONTEXT = 32


def draw_decay_rate(key, part):
    pick_key, fast_key, middle_key, slow_key = jax.random.split(key, 4)
    fast_share = 0.2
    middle_share = 0.3
    picked = jax.random.uniform(pick_key, (2, HEADS), jnp.float32)
    fast_rate = jnp.exp(jax.random.uniform(fast_key, (2, HEADS), jnp.float32, math.log(1.0 / 50.0), math.log(1.0 / 30.0)))
    middle_rate = jnp.exp(jax.random.uniform(middle_key, (2, HEADS), jnp.float32, math.log(0.001), math.log(0.01)))
    slow_rate = jnp.exp(jax.random.uniform(slow_key, (2, HEADS), jnp.float32, math.log(0.05 / LATENT_TOKENS), math.log(0.3 / LATENT_TOKENS)))
    return jnp.where(picked < fast_share, fast_rate, jnp.where(picked < fast_share + middle_share, middle_rate, slow_rate))


def draw_extra_decay(key, part):
    rate_key, place_key, depth_key = jax.random.split(key, 3)
    span_count = LATENT_TOKENS // TOK_DEV
    block_rates = jnp.exp(jax.random.uniform(rate_key, (SAMPLES, 2, HEADS, span_count), jnp.float32, math.log(0.1 / LATENT_TOKENS), math.log(0.6 / LATENT_TOKENS)))
    steady_state = -jnp.repeat(block_rates, TOK_DEV, axis=-1)
    third_len = LATENT_TOKENS // 3
    offsets = jax.random.randint(place_key, (SAMPLES, 2, HEADS, 3), 0, third_len)
    token_places = offsets + third_len * jnp.arange(3)
    depth_values = jnp.log(jax.random.uniform(depth_key, (SAMPLES, 2, HEADS, 3), jnp.float32, 0.5, 0.8))
    impulse_matches = (jnp.arange(LATENT_TOKENS)[None, None, None, None, :] == token_places[..., None]).astype(jnp.float32)
    return steady_state + jnp.sum(impulse_matches * depth_values[..., None], axis=-2)


def shard_levels(rng, dims, cuts, least, top_value):
    def one(axis_at, blocks):
        steps = jax.random.uniform(jax.random.fold_in(jax.random.fold_in(rng, 6), axis_at), (blocks,), jnp.float32, least / len(cuts), top_value / len(cuts))
        return jnp.repeat(jnp.exp(steps), dims[axis_at] // blocks).reshape((-1,) + (1,) * (len(dims) - axis_at - 1))

    factor_of = one(*cuts[0])
    for cut in cuts[1:]:
        factor_of = factor_of * one(*cut)
    return factor_of


def centred(rng, extent, deviation, most, cuts=(), kind=jnp.bfloat16):
    entries = deviation * jax.random.normal(rng, extent, jnp.float32)
    if cuts:
        entries = entries * shard_levels(rng, extent, cuts, -0.22, 0.18)
    return jnp.clip(entries, -most, most).astype(kind)


def setup_inputs(seed: int = 0) -> dict:
    seeds = jax.random.split(jax.random.key(seed), 18)
    return {
        "latent": centred(seeds[0], (SAMPLES, LATENT_TOKENS, D), 1.0, 6.0, ((0, 2), (1, 4))),
        "cond": centred(seeds[1], (SAMPLES, D), 1.0, 6.0, ((0, 2), (1, 4))),
        "context": centred(seeds[2], (SAMPLES, CONTEXT, D), 1.0, 6.0, ((0, 2), (1, 4))),
        "ctx_cond": centred(seeds[3], (D,), 1.0, 6.0, ((0, 4),)),
        "w_mod": centred(seeds[4], (D, 3 * D), D ** -0.5, 0.125, ((0, 4), (1, 4))),
        "norm_gain": jnp.clip(1.0 + 0.18 * jax.random.normal(seeds[5], (D,), jnp.float32), 0.099609375, 1.8984375).astype(jnp.bfloat16),
        "w_query": centred(seeds[6], (D, HEADS * HEAD), D ** -0.5, 0.125, ((1, 4),)),
        "w_key": centred(seeds[7], (D, HEADS * HEAD), D ** -0.5, 0.125, ((1, 4),)),
        "w_value": centred(seeds[8], (D, HEADS * HEAD), D ** -0.5, 0.125, ((1, 4),)),
        "w_outgate": centred(seeds[9], (D, HEADS * HEAD), D ** -0.5, 0.125, ((1, 4),)),
        "w_decay": centred(seeds[10], (D, 2, HEADS), D ** -0.5, 0.125, ((2, 4),)),
        "w_beta": centred(seeds[11], (D, 2, HEADS), D ** -0.5, 0.125, ((2, 4),)),
        "decay_rate": draw_decay_rate(jax.random.fold_in(seeds[17], 71), 0),
        "decay_bias": centred(seeds[13], (2, HEADS), 1.0, 3.0, ((1, 4),), jnp.float32),
        "extra_decay": draw_extra_decay(jax.random.fold_in(seeds[17], 71), 0),
        "out_gain": jnp.clip(1.0 + 0.18 * jax.random.normal(seeds[15], (HEAD,), jnp.float32), 0.099609375, 1.8984375).astype(jnp.bfloat16),
        "w_out": centred(seeds[16], (HEADS * HEAD, D), (HEADS * HEAD) ** -0.5, 0.1875),
    }


norm_eps = 1e-06
beta_scale = 30.0

def contract_product(einsum_form, left_op, right_op):
    return jnp.einsum(einsum_form, left_op, right_op, precision=lax.Precision.HIGHEST)

def modulate(rows_in, gain_vec, scale_row, shift_row):
    values = rows_in.astype(jnp.float32)
    normed = values * lax.rsqrt(lax.optimization_barrier(jnp.mean(values * values, axis=-1, keepdims=True)) + norm_eps)
    return (normed * gain_vec.astype(jnp.float32) * (1.0 + scale_row) + shift_row).astype(jnp.bfloat16)

def unit_normal(values):
    return values * lax.rsqrt(lax.optimization_barrier(jnp.sum(values * values, axis=-1, keepdims=True)) + norm_eps)

def head_view(raw_proj, head_count):
    return raw_proj.astype(jnp.float32).reshape(raw_proj.shape[0], head_count, -1)

def split_inputs(raw_proj, head_count, inner_width):
    row_count = raw_proj.shape[0]
    key_rows = unit_normal(jax.nn.silu(head_view(raw_proj[:, :inner_width], head_count)))
    value_rows = jax.nn.silu(head_view(raw_proj[:, inner_width:2 * inner_width], head_count))
    decay_raw = raw_proj[:, 2 * inner_width:2 * inner_width + 2 * head_count].astype(jnp.float32)
    beta_raw = raw_proj[:, 2 * inner_width + 2 * head_count:].astype(jnp.float32)
    return (key_rows, value_rows, decay_raw.reshape(row_count, 2, head_count), beta_raw.reshape(row_count, 2, head_count))

def orient(values, direction):
    if direction:
        return values[::-1]
    return values

def to_blocks(values, block_width):
    block_count = values.shape[0] // block_width
    shaped = values.reshape((block_count, block_width) + values.shape[1:])
    return jnp.moveaxis(shaped, 2, 1)

def unit_inverse(lowpart, block_width):
    positions = jnp.arange(block_width)
    result = jnp.broadcast_to(jnp.eye(block_width, dtype=jnp.float32), lowpart.shape)
    for level_index in range((block_width - 1).bit_length()):
        half_width = 1 << level_index
        same_pair = positions[:, None] // (2 * half_width) == positions[None, :] // (2 * half_width)
        lower_half = positions[:, None] // half_width % 2 == 1
        upper_half = positions[None, :] // half_width % 2 == 0
        coupling = jnp.where(same_pair & lower_half & upper_half, lowpart, 0.0)
        result = result - contract_product('nhij,nhjk->nhik', result, contract_product('nhij,nhjk->nhik', coupling, result))
    return result

def block_terms(key_rows, value_rows, log_decay, beta_rows, block_width):
    key_blocks = to_blocks(key_rows, block_width)
    value_blocks = to_blocks(value_rows, block_width)
    cumulative = jnp.cumsum(to_blocks(log_decay, block_width), axis=-1)
    beta_blocks = to_blocks(beta_rows, block_width)
    positions = jnp.arange(block_width)
    lower_mask = positions[:, None] >= positions[None, :]
    strict = positions[:, None] > positions[None, :]
    spread = cumulative[..., :, None] - cumulative[..., None, :]
    weights = jnp.where(lower_mask, jnp.exp(jnp.where(lower_mask, spread, 0.0)), 0.0)
    scaled = key_blocks * beta_blocks[..., None]
    lowpart = jnp.where(strict, contract_product('nhid,nhjd->nhij', scaled, key_blocks) * weights, 0.0)
    inverse = unit_inverse(lowpart, block_width)
    state_update = contract_product('nhij,nhjd->nhid', inverse, value_blocks * beta_blocks[..., None])
    erased_state = contract_product('nhij,nhjd->nhid', inverse, scaled * jnp.exp(cumulative)[..., None])
    final_log_decay = cumulative[..., -1]
    decayed_keys = key_blocks * jnp.exp(final_log_decay[..., None] - cumulative)[..., None]
    return ((state_update, erased_state, decayed_keys, final_log_decay), (key_blocks, cumulative, weights))

def query_terms(queries, extras):
    key_blocks, cumulative, weights = extras
    query_blocks = to_blocks(queries, key_blocks.shape[2])
    query_decayed = query_blocks * jnp.exp(cumulative)[..., None]
    query_keys = contract_product('nhid,nhjd->nhij', query_blocks, key_blocks) * weights
    return (query_decayed, query_keys)

def direction_terms(key_rows, value_rows, decay_raw, beta_raw, decay_rate, decay_bias, direction, added, block_width):
    log_decay = -decay_rate[direction] * jax.nn.softplus(decay_raw[:, direction] + decay_bias[direction]) + added
    beta_rows = jax.nn.sigmoid(beta_raw[:, direction]) * (beta_scale * decay_rate[direction])
    return block_terms(orient(key_rows, direction), orient(value_rows, direction), orient(log_decay, direction), orient(beta_rows, direction), block_width)

def carry_state(state_now, parts):

    def advance(carried_state, inputs):
        state_update, erased_state, decayed_keys, final_log_decay = inputs
        new_value_rows = state_update - contract_product('tze,tem->tzm', erased_state, carried_state)
        carried_state = carried_state * jnp.exp(final_log_decay)[:, None, None] + contract_product('rbz,rbi->rzi', decayed_keys, new_value_rows)
        return (carried_state, None)
    return lax.scan(advance, state_now, parts)[0]

def read_out(state_now, parts, query_decayed, query_keys):

    def advance(carried_state, inputs):
        state_update, erased_state, decayed_keys, final_log_decay, query_tile, query_matrix = inputs
        new_value_rows = state_update - contract_product('tze,tem->tzm', erased_state, carried_state)
        state_readout = contract_product('tze,tem->tzm', query_tile, carried_state) + contract_product('bgd,bdc->bgc', query_matrix, new_value_rows)
        carried_state = carried_state * jnp.exp(final_log_decay)[:, None, None] + contract_product('rbz,rbi->rzi', decayed_keys, new_value_rows)
        return (carried_state, state_readout)
    readouts = lax.scan(advance, state_now, parts + (query_decayed, query_keys))[1]
    block_count, head_count, block_width, value_width = readouts.shape
    return jnp.moveaxis(readouts, 1, 2).reshape(block_count * block_width, head_count, value_width)

def reference(latent, cond, context, ctx_cond, w_mod, norm_gain, w_query, w_key, w_value, w_outgate, w_decay, w_beta, decay_rate, decay_bias, extra_decay, out_gain, w_out):
    inner_width = HEADS * HEAD
    cond_all = jnp.concatenate([cond, ctx_cond[None, :]], axis=0)
    cond_rows = jax.nn.silu(cond_all.astype(jnp.float32)).astype(jnp.bfloat16)
    modulation = jnp.dot(cond_rows, w_mod, preferred_element_type=jnp.float32)
    shift_rows = modulation[:, :D]
    scale_rows = modulation[:, D:2 * D]
    gate_rows = modulation[:, 2 * D:]
    ctx_joined = jnp.concatenate([w_key, w_value, w_decay.reshape(D, 2 * HEADS), w_beta.reshape(D, 2 * HEADS)], axis=1)
    lat_joined = jnp.concatenate([w_query, w_outgate, ctx_joined], axis=1)
    zero_state = jnp.zeros((HEADS, HEAD, HEAD), jnp.float32)
    ctx_block = min(BLOCK, CONTEXT)
    results = []
    for sample in range(SAMPLES):
        ctx_in = modulate(context[sample], norm_gain, scale_rows[SAMPLES], shift_rows[SAMPLES])
        ctx_proj = jnp.dot(ctx_in, ctx_joined, preferred_element_type=jnp.float32).astype(jnp.bfloat16)
        lat_in = modulate(latent[sample], norm_gain, scale_rows[sample], shift_rows[sample])
        lat_proj = jnp.dot(lat_in, lat_joined, preferred_element_type=jnp.float32).astype(jnp.bfloat16)
        queries = unit_normal(jax.nn.silu(head_view(lat_proj[:, :inner_width], HEADS))) * HEAD ** (-0.5)
        outgate = lat_proj[:, inner_width:2 * inner_width]
        ctx_inputs = split_inputs(ctx_proj, HEADS, inner_width)
        lat_inputs = split_inputs(lat_proj[:, 2 * inner_width:], HEADS, inner_width)
        summed_out = jnp.zeros((LATENT_TOKENS, HEADS, HEAD), jnp.float32)
        for direction in range(2):
            ctx_parts = direction_terms(*ctx_inputs, decay_rate, decay_bias, direction, 0.0, ctx_block)[0]
            ctx_state = carry_state(zero_state, ctx_parts)
            lat_parts, extras = direction_terms(*lat_inputs, decay_rate, decay_bias, direction, extra_decay[sample, direction].T, BLOCK)
            query_decayed, query_keys = query_terms(orient(queries, direction), extras)
            summed_out = summed_out + orient(read_out(ctx_state, lat_parts, query_decayed, query_keys), direction)
        normed = summed_out * lax.rsqrt(lax.optimization_barrier(jnp.mean(summed_out * summed_out, axis=-1, keepdims=True)) + norm_eps)
        normed = normed * out_gain.astype(jnp.float32)
        gated = (normed * jax.nn.silu(head_view(outgate, HEADS))).reshape(LATENT_TOKENS, inner_width).astype(jnp.bfloat16)
        mixed_rows = jnp.dot(gated, w_out, preferred_element_type=jnp.float32)
        results.append((latent[sample].astype(jnp.float32) + gate_rows[sample] * mixed_rows).astype(jnp.bfloat16))
    return jnp.stack(results)
```

```python
import functools

import jax
import jax.numpy as jnp
from jax import lax
from jax.experimental import pallas as pl
from jax.experimental.pallas import tpu as pltpu
from jax.sharding import PartitionSpec as P

HEAD = 128
norm_eps = 1e-06
beta_scale = 30.0
MESH = pl.DeviceIdType.MESH
F32 = jnp.float32
BF16 = jnp.bfloat16


def mm(a, b):
    return jnp.dot(a.astype(BF16), b.astype(BF16), preferred_element_type=F32)


def mm_nt(a, b):
    return lax.dot_general(
        a.astype(BF16), b.astype(BF16), (((1,), (1,)), ((), ())), preferred_element_type=F32
    )


def silu(v):
    return v / (1.0 + jnp.exp(-v))


def unit_normal(u):
    return u * lax.rsqrt(jnp.sum(u * u, axis=-1, keepdims=True) + norm_eps)


def softplus(v):
    return jnp.maximum(v, 0.0) + jnp.log1p(jnp.exp(-jnp.abs(v)))


def kernel(
    n,
    t,
    heads,
    rate_ref,
    bias_ref,
    cond_ref,
    ctx_cond_ref,
    context_ref,
    gain_ref,
    out_gain_ref,
    wdb_ref,
    extra_ref,
    latent_hbm,
    w_mod_hbm,
    w_query_hbm,
    w_outgate_hbm,
    w_key_hbm,
    w_value_hbm,
    w_out_hbm,
    out_ref,
    lat_v,
    wm_v,
    w_v,
    wout_v,
    ctx_all,
    mod_part,
    mod_full,
    xin,
    ext_v,
    own_a,
    own_b,
    pre_a,
    pre_b,
    send_map,
    recv_map,
    gated_v,
    gated_r,
    load_sem,
    ctx_send,
    ctx_recv,
    part_send,
    part_recv,
    full_send,
    full_recv,
    map_send,
    map_recv,
    gate_send,
    gate_recv,
):
    sp = lax.axis_index("sp")
    tp = lax.axis_index("tp")
    span = lat_v.shape[0]
    depth = lat_v.shape[1]
    rows = xin.shape[0]
    ctx_len = n * context_ref.shape[1]
    inner = heads * HEAD
    chains = 2 * heads
    rows_out = span // t

    def load(i, src, dst):
        copy = pltpu.make_async_copy(src, dst, load_sem.at[i])
        copy.start()
        return copy

    load_mod = load(0, w_mod_hbm, wm_v)
    load_lat = load(1, latent_hbm.at[0], lat_v)
    load_w = [
        load(2 + i, w, w_v.at[i])
        for i, w in enumerate((w_key_hbm, w_value_hbm, w_query_hbm, w_outgate_hbm))
    ]
    load_out = load(6, w_out_hbm, wout_v)

    barrier = pltpu.get_barrier_semaphore()
    for k in range(1, n):
        pl.semaphore_signal(
            barrier, inc=1, device_id={"sp": lax.rem(sp + k, n)}, device_id_type=MESH
        )
    for k in range(1, t):
        pl.semaphore_signal(
            barrier, inc=1, device_id={"tp": lax.rem(tp + k, t)}, device_id_type=MESH
        )
    pl.semaphore_wait(barrier, n + t - 2)

    def spread(axis, me, count, src, dst, send, recv):
        sent = []
        for k in range(1, count):
            copy = pltpu.make_async_remote_copy(
                src_ref=src,
                dst_ref=dst.at[me],
                send_sem=send.at[k],
                recv_sem=recv.at[k],
                device_id={axis: lax.rem(me + k, count)},
                device_id_type=MESH,
            )
            copy.start()
            sent.append(copy)
        return sent

    def collect(axis, me, count, dst, send, recv):
        for k in range(1, count):
            slot = dst.at[lax.rem(me + count - k, count)]
            pltpu.make_async_remote_copy(
                src_ref=slot,
                dst_ref=slot,
                send_sem=send.at[k],
                recv_sem=recv.at[k],
                device_id={axis: lax.rem(me + k, count)},
                device_id_type=MESH,
            ).wait_recv()

    ctx_sent = spread("sp", sp, n, context_ref.at[0], ctx_all, ctx_send, ctx_recv)
    ctx_all[sp] = context_ref[0]

    pick = lax.broadcasted_iota(jnp.int32, (8, 1), 0)
    cond_f = silu(cond_ref[...].astype(F32))
    ctx_cond_f = silu(ctx_cond_ref[...].astype(F32))
    cond_rows = jnp.where(pick == 0, cond_f, jnp.where(pick == 1, ctx_cond_f, 0.0)).astype(BF16)
    load_mod.wait()
    part = jnp.dot(cond_rows, wm_v[...], preferred_element_type=F32)
    mod_part[sp] = part[:2]
    part_sent = spread("sp", sp, n, mod_part.at[sp], mod_part, part_send, part_recv)

    load_lat.wait()
    lat = lat_v[...].astype(F32)
    lat_r = lax.rsqrt(jnp.mean(lat * lat, axis=-1, keepdims=True) + norm_eps)
    collect("sp", sp, n, ctx_all, ctx_send, ctx_recv)
    ctx = ctx_all[...].astype(F32).reshape(ctx_len, depth)
    ctx_r = lax.rsqrt(jnp.mean(ctx * ctx, axis=-1, keepdims=True) + norm_eps)
    gain = gain_ref[...].astype(F32)
    if rows > span + ctx_len:
        xin[span + ctx_len :, :] = jnp.zeros((rows - span - ctx_len, depth), BF16)
    ext_v[...] = jnp.zeros(ext_v.shape, F32)
    for d in range(2):
        ext_v[d * heads : (d + 1) * heads, :span] = extra_ref[0, d]

    collect("sp", sp, n, mod_part, part_send, part_recv)
    summed = mod_part[0]
    for j in range(1, n):
        summed = summed + mod_part[j]
    mod_full[tp] = summed
    full_sent = spread("tp", tp, t, mod_full.at[tp], mod_full, full_send, full_recv)

    at_row = lax.broadcasted_iota(jnp.int32, (rows, rows), 0)
    at_col = lax.broadcasted_iota(jnp.int32, (rows, rows), 1)
    same = (at_row < span) == (at_col < span)
    lane = lax.broadcasted_iota(jnp.int32, (1, rows), 1)
    is_lat = lane < span
    is_ctx = jnp.logical_and(lane >= span, lane < span + ctx_len)

    collect("tp", tp, t, mod_full, full_send, full_recv)
    modulation = jnp.concatenate([mod_full[j] for j in range(t)], axis=1)
    shift = modulation[:, :depth]
    scale = gain * (1.0 + modulation[:, depth : 2 * depth])
    gate = modulation[0:1, 2 * depth :]
    xin[:span, :] = (lat_v[...].astype(F32) * lat_r * scale[0:1] + shift[0:1]).astype(BF16)
    ctx = ctx_all[...].astype(F32).reshape(ctx_len, depth)
    xin[span : span + ctx_len, :] = (ctx * ctx_r * scale[1:2] + shift[1:2]).astype(BF16)

    raw_t = lax.dot_general(
        wdb_ref[...], xin[...], (((1,), (1,)), ((), ())), preferred_element_type=F32
    ).astype(BF16).astype(F32)

    def project(i):
        load_w[i].wait()
        return jnp.dot(xin[...], w_v[i], preferred_element_type=F32).astype(BF16).astype(F32)

    chain = lax.broadcasted_iota(jnp.int32, (chains, 1), 0)
    rate = jnp.zeros((chains, 1), F32)
    bias = jnp.zeros((chains, 1), F32)
    for c in range(chains):
        rate = jnp.where(chain == c, rate_ref[c // heads, c % heads], rate)
        bias = jnp.where(chain == c, bias_ref[c // heads, c % heads], bias)
    g = -rate * softplus(raw_t[:chains] + bias) + ext_v[:chains, :]
    g = jnp.where(jnp.logical_or(is_lat, is_ctx), g, 0.0)
    beta = beta_scale * rate / (1.0 + jnp.exp(-raw_t[chains : 2 * chains]))
    up_to = jnp.where(jnp.logical_and(same, at_row <= at_col), 1.0, 0.0)
    from_on = jnp.where(jnp.logical_and(same, at_row >= at_col), 1.0, 0.0)
    g_hi = g.astype(BF16).astype(F32)
    g_mid = (g - g_hi).astype(BF16).astype(F32)
    g_lo = g - g_hi - g_mid
    g_parts = jnp.concatenate([g_hi, g_mid, g_lo, jnp.zeros_like(g)], axis=0)
    sums_0 = mm(g_parts, up_to)
    sums_1 = mm(g_parts, from_on)

    def join(s):
        return s[:chains] + s[chains : 2 * chains] + s[2 * chains : 3 * chains]

    cum = jnp.where(chain < heads, join(sums_0), join(sums_1))
    tot_lat = jnp.sum(jnp.where(is_lat, g, 0.0), axis=-1, keepdims=True)
    tot_ctx = jnp.sum(jnp.where(is_ctx, g, 0.0), axis=-1, keepdims=True)
    to_end_lat = jnp.where(is_lat, jnp.exp(jnp.where(is_lat, tot_lat - cum, 0.0)), 0.0)
    to_end_ctx = jnp.where(is_ctx, jnp.exp(jnp.where(is_ctx, tot_ctx - cum, 0.0)), 0.0)
    through = jnp.exp(tot_lat)
    packed = jnp.concatenate(
        [cum, beta, jnp.zeros((HEAD - 2 * chains, rows), F32)], axis=0
    )
    cols = packed.T
    grow = jnp.exp(cols)

    key_raw, value_raw = project(0), project(1)
    keys, values, queries, keys_t = [], [], [], []
    for h in range(heads):
        part_h = slice(h * HEAD, (h + 1) * HEAD)
        k = unit_normal(silu(key_raw[:, part_h]))
        keys.append(k)
        keys_t.append(k.T)
        values.append(silu(value_raw[:, part_h]))
    kk = [mm_nt(k, k) for k in keys]

    tri = [at_row >= at_col, at_row <= at_col]
    weights, low, inv = [], [], []
    for c in range(chains):
        d, h = c // heads, c % heads
        mask = jnp.logical_and(same, tri[d])
        diff = cols[:, c : c + 1] - cum[c : c + 1, :]
        w = jnp.where(mask, jnp.exp(jnp.where(mask, diff, 0.0)), 0.0)
        weights.append(w)
        b = cols[:, chains + c : chains + c + 1]
        low.append(jnp.where(at_row != at_col, b * kk[h] * w, 0.0))
    half = 1
    while half < rows:
        pair = at_row // (2 * half) == at_col // (2 * half)
        cross = [
            jnp.logical_and(pair, jnp.logical_and(at_row // half % 2 == 1, at_col // half % 2 == 0)),
            jnp.logical_and(pair, jnp.logical_and(at_row // half % 2 == 0, at_col // half % 2 == 1)),
        ]
        coupling = [jnp.where(cross[c // heads], low[c], 0.0) for c in range(chains)]
        if half == 1:
            eye = jnp.where(at_row == at_col, 1.0, 0.0)
            inv = [eye - coupling[c] for c in range(chains)]
        else:
            inner_term = [mm(coupling[c], inv[c]) for c in range(chains)]
            inv = [inv[c] - mm(inv[c], inner_term[c]) for c in range(chains)]
        half *= 2

    eye_head = jnp.where(
        lax.broadcasted_iota(jnp.int32, (HEAD, HEAD), 0)
        == lax.broadcasted_iota(jnp.int32, (HEAD, HEAD), 1),
        1.0,
        0.0,
    )
    solved = []
    place = [sp, n - 1 - sp]
    for c in range(chains):
        d, h = c // heads, c % heads
        b = cols[:, chains + c : chains + c + 1]
        right = jnp.concatenate(
            [values[h] * b, keys[h] * (b * grow[:, c : c + 1])], axis=1
        )
        x = mm(inv[c], right)
        solved.append(x)
        ba = mm(keys_t[h] * to_end_lat[c : c + 1, :], x)
        ctx_state = mm(keys_t[h] * to_end_ctx[c : c + 1, :], x[:, :HEAD])
        a = eye_head * through[c : c + 1, :] - ba[:, HEAD:]
        b_map = ba[:, :HEAD]
        first = place[d] == 0
        own_a[c] = a
        own_b[c] = b_map
        pre_a[c] = jnp.where(first, 0.0, eye_head)
        pre_b[c] = jnp.where(first, ctx_state, 0.0)
        send_map[0, d, h] = jnp.where(first, 0.0, a).astype(BF16)
        send_map[0, d, heads + h] = (
            b_map + jnp.where(first, mm(a, ctx_state), 0.0)
        ).astype(BF16)

    def map_copy(level, d, k):
        wide = 1 << level
        low_at = heads if 2 * wide == n else 0
        part_of = pl.ds(low_at, 2 * heads - low_at)
        target = lax.rem(sp + k, n) if d == 0 else lax.rem(sp + n - k, n)
        return pltpu.make_async_remote_copy(
            src_ref=send_map.at[level, d, part_of],
            dst_ref=recv_map.at[level, d, part_of],
            send_sem=map_send.at[level, d, k],
            recv_sem=map_recv.at[level, d],
            device_id={"sp": target},
            device_id_type=MESH,
        )

    levels = (n - 1).bit_length()

    def send_level(level):
        wide = 1 << level
        for d in range(2):

            @pl.when(lax.rem(place[d], 2 * wide) == wide - 1)
            def _():
                if level:
                    for h in range(heads):
                        c = d * heads + h
                        a = own_a[c]
                        send_map[level, d, heads + h] = (
                            mm(a, pre_b[c]) + own_b[c]
                        ).astype(BF16)
                        if 2 * wide != n:
                            send_map[level, d, h] = mm(a, pre_a[c]).astype(BF16)
                for k in range(1, wide + 1):
                    map_copy(level, d, k).start()

    def recv_level(level):
        wide = 1 << level
        for d in range(2):

            @pl.when(lax.rem(place[d], 2 * wide) >= wide)
            def _():
                map_copy(level, d, 1).wait_recv()
                for h in range(heads):
                    c = d * heads + h
                    a = pre_a[c]
                    pre_b[c] = mm(a, recv_map[level, d, heads + h]) + pre_b[c]
                    if 2 * wide != n:
                        pre_a[c] = mm(a, recv_map[level, d, h])

    if levels:
        send_level(0)

    query_raw, outgate_raw = project(2), project(3)
    local, mixers = [], []
    for h in range(heads):
        part_h = slice(h * HEAD, (h + 1) * HEAD)
        q = unit_normal(silu(query_raw[:, part_h])) * HEAD ** (-0.5)
        qk = mm_nt(q, keys[h])
        read = [mm(qk * weights[d * heads + h], solved[d * heads + h]) for d in range(2)]
        local.append(read[0][:, :HEAD] + read[1][:, :HEAD])
        mixers.append(
            jnp.concatenate(
                [
                    q * grow[:, d * heads + h : d * heads + h + 1] - read[d][:, HEAD:]
                    for d in range(2)
                ],
                axis=1,
            )
        )

    out_gate = [silu(outgate_raw[:, h * HEAD : (h + 1) * HEAD]) for h in range(heads)]
    for level in range(levels):
        recv_level(level)
        if level + 1 < levels:
            send_level(level + 1)

    out_gain = out_gain_ref[...].astype(F32)
    for h in range(heads):
        state = jnp.concatenate([pre_b[h], pre_b[heads + h]], axis=0)
        o = local[h] + mm(mixers[h], state)
        normed = o * lax.rsqrt(jnp.mean(o * o, axis=-1, keepdims=True) + norm_eps)
        gated = (normed * out_gain * out_gate[h]).astype(BF16)
        for j in range(t):
            gated_v[j, :, h * HEAD : (h + 1) * HEAD] = gated[j * rows_out : (j + 1) * rows_out]

    gate_sent = []
    for k in range(1, t):
        target = lax.rem(tp + k, t)
        copy = pltpu.make_async_remote_copy(
            src_ref=gated_v.at[target],
            dst_ref=gated_r.at[tp],
            send_sem=gate_send.at[k],
            recv_sem=gate_recv.at[k],
            device_id={"tp": target},
            device_id_type=MESH,
        )
        copy.start()
        gate_sent.append(copy)
    gated_r[tp] = gated_v[tp]
    load_out.wait()
    collect("tp", tp, t, gated_r, gate_send, gate_recv)
    by_rows = jnp.concatenate([gated_r[j] for j in range(t)], axis=1)
    mixed = jnp.dot(by_rows, wout_v[...], preferred_element_type=F32)
    own_rows = lat_v[pl.ds(pl.multiple_of(tp * rows_out, rows_out), rows_out), :].astype(F32)
    out_ref[0] = (own_rows + gate * mixed).astype(out_ref.dtype)

    for copy in ctx_sent + part_sent + full_sent + gate_sent:
        copy.wait_send()
    for level in range(levels):
        wide = 1 << level
        for d in range(2):

            @pl.when(lax.rem(place[d], 2 * wide) == wide - 1)
            def _():
                for k in range(1, wide + 1):
                    map_copy(level, d, k).wait_send()


def on_device(
    n,
    t,
    latent,
    cond,
    context,
    ctx_cond,
    w_mod,
    norm_gain,
    w_query,
    w_key,
    w_value,
    w_outgate,
    w_decay,
    w_beta,
    decay_rate,
    decay_bias,
    extra_decay,
    out_gain,
    w_out,
):
    depth = latent.shape[2]
    span = latent.shape[1]
    heads = w_decay.shape[2]
    inner = heads * HEAD
    chains = 2 * heads
    ctx_len = n * context.shape[1]
    rows = -(-(span + ctx_len) // 128) * 128
    rows_out = span // t
    levels = max(1, (n - 1).bit_length())
    wdb = jnp.concatenate([w_decay.reshape(depth, chains), w_beta.reshape(depth, chains)], axis=1).T
    vmem = pl.BlockSpec(memory_space=pltpu.VMEM)
    smem = pl.BlockSpec(memory_space=pltpu.SMEM)
    hbm = pl.BlockSpec(memory_space=pl.ANY)
    dma = pltpu.SemaphoreType.DMA
    return pl.pallas_call(
        functools.partial(kernel, n, t, heads),
        out_shape=jax.ShapeDtypeStruct((1, rows_out, depth), BF16),
        in_specs=[smem] * 2 + [vmem] * 7 + [hbm] * 7,
        out_specs=vmem,
        scratch_shapes=[
            pltpu.VMEM((span, depth), BF16),
            pltpu.VMEM(w_mod.shape, BF16),
            pltpu.VMEM((4, depth, inner), BF16),
            pltpu.VMEM(w_out.shape, BF16),
            pltpu.VMEM((n,) + context.shape[1:], BF16),
            pltpu.VMEM((n, 2, w_mod.shape[1]), F32),
            pltpu.VMEM((t, 2, w_mod.shape[1]), F32),
            pltpu.VMEM((rows, depth), BF16),
            pltpu.VMEM((8, rows), F32),
            pltpu.VMEM((chains, HEAD, HEAD), F32),
            pltpu.VMEM((chains, HEAD, HEAD), F32),
            pltpu.VMEM((chains, HEAD, HEAD), F32),
            pltpu.VMEM((chains, HEAD, HEAD), F32),
            pltpu.VMEM((levels, 2, 2 * heads, HEAD, HEAD), BF16),
            pltpu.VMEM((levels, 2, 2 * heads, HEAD, HEAD), BF16),
            pltpu.VMEM((t, rows_out, inner), BF16),
            pltpu.VMEM((t, rows_out, inner), BF16),
            dma((7,)),
            dma((n,)),
            dma((n,)),
            dma((n,)),
            dma((n,)),
            dma((t,)),
            dma((t,)),
            dma((levels, 2, n)),
            dma((levels, 2)),
            dma((t,)),
            dma((t,)),
        ],
        compiler_params=pltpu.CompilerParams(
            collective_id=0, has_side_effects=True, vmem_limit_bytes=60 * 1024 * 1024
        ),
    )(
        decay_rate,
        decay_bias,
        cond,
        ctx_cond[None, :],
        context,
        norm_gain[None, :],
        out_gain[None, :],
        wdb,
        extra_decay,
        latent,
        w_mod,
        w_query,
        w_outgate,
        w_key,
        w_value,
        w_out,
    )


def solution(mesh):
    placed = (
        P("dp", "sp", None),
        P("dp", "sp"),
        P("dp", "sp", None),
        P("sp"),
        P("sp", "tp"),
        P(),
        P(None, "tp"),
        P(None, "tp"),
        P(None, "tp"),
        P(None, "tp"),
        P(None, None, "tp"),
        P(None, None, "tp"),
        P(None, "tp"),
        P(None, "tp"),
        P("dp", None, "tp", "sp"),
        P(),
        P(),
    )
    return jax.shard_map(
        functools.partial(on_device, mesh.shape["sp"], mesh.shape["tp"]),
        mesh=mesh,
        in_specs=placed,
        out_specs=P("dp", ("sp", "tp"), None),
        check_vma=False,
    )
```

```python
import functools

import jax
import jax.numpy as jnp
from jax import lax
from jax.experimental import pallas as pl
from jax.experimental.pallas import tpu as pltpu
from jax.sharding import PartitionSpec as P

HEAD = 128
norm_eps = 1e-06
beta_scale = 30.0
MESH = pl.DeviceIdType.MESH
F32 = jnp.float32
BF16 = jnp.bfloat16


def mm(a, b):
    return jnp.dot(a.astype(BF16), b.astype(BF16), preferred_element_type=F32)


def mm_nt(a, b):
    return lax.dot_general(
        a.astype(BF16), b.astype(BF16), (((1,), (1,)), ((), ())), preferred_element_type=F32
    )


def silu(v):
    return v / (1.0 + jnp.exp(-v))


def unit_normal(u):
    return u * lax.rsqrt(jnp.sum(u * u, axis=-1, keepdims=True) + norm_eps)


def softplus(v):
    return jnp.maximum(v, 0.0) + jnp.log1p(jnp.exp(-jnp.abs(v)))


def kernel(
    n,
    t,
    heads,
    rate_ref,
    bias_ref,
    cond_ref,
    ctx_cond_ref,
    context_ref,
    gain_ref,
    out_gain_ref,
    w_decay_ref,
    w_beta_ref,
    extra_ref,
    latent_hbm,
    w_mod_hbm,
    w_query_hbm,
    w_outgate_hbm,
    w_key_hbm,
    w_value_hbm,
    w_out_hbm,
    out_ref,
    lat_v,
    wm_v,
    w_v,
    wout_v,
    ctx_all,
    mod_part,
    mod_full,
    xin,
    ext_v,
    own_a,
    own_b,
    pre_a,
    pre_b,
    send_map,
    recv_map,
    gated_v,
    gated_r,
    load_sem,
    ctx_send,
    ctx_recv,
    part_send,
    part_recv,
    full_send,
    full_recv,
    map_send,
    map_recv,
    gate_send,
    gate_recv,
):
    sp = lax.axis_index("sp")
    tp = lax.axis_index("tp")
    span = lat_v.shape[0]
    depth = lat_v.shape[1]
    rows = xin.shape[0]
    ctx_len = n * context_ref.shape[1]
    inner = heads * HEAD
    chains = 2 * heads
    rows_out = span // t

    def load(i, src, dst):
        copy = pltpu.make_async_copy(src, dst, load_sem.at[i])
        copy.start()
        return copy

    load_mod = load(0, w_mod_hbm, wm_v)
    load_lat = load(1, latent_hbm.at[0], lat_v)

    barrier = pltpu.get_barrier_semaphore()
    for k in range(1, n):
        pl.semaphore_signal(
            barrier, inc=1, device_id={"sp": lax.rem(sp + k, n)}, device_id_type=MESH
        )
    for k in range(1, t):
        pl.semaphore_signal(
            barrier, inc=1, device_id={"tp": lax.rem(tp + k, t)}, device_id_type=MESH
        )
    pl.semaphore_wait(barrier, n + t - 2)

    def spread(axis, me, count, src, dst, send, recv):
        sent = []
        for k in range(1, count):
            copy = pltpu.make_async_remote_copy(
                src_ref=src,
                dst_ref=dst.at[me],
                send_sem=send.at[k],
                recv_sem=recv.at[k],
                device_id={axis: lax.rem(me + k, count)},
                device_id_type=MESH,
            )
            copy.start()
            sent.append(copy)
        return sent

    def collect(axis, me, count, dst, send, recv):
        for k in range(1, count):
            slot = dst.at[lax.rem(me + count - k, count)]
            pltpu.make_async_remote_copy(
                src_ref=slot,
                dst_ref=slot,
                send_sem=send.at[k],
                recv_sem=recv.at[k],
                device_id={axis: lax.rem(me + k, count)},
                device_id_type=MESH,
            ).wait_recv()

    ctx_sent = spread("sp", sp, n, context_ref.at[0], ctx_all, ctx_send, ctx_recv)
    ctx_all[sp] = context_ref[0]

    pick = lax.broadcasted_iota(jnp.int32, (8, 1), 0)
    cond_f = silu(cond_ref[...].astype(F32))
    ctx_cond_f = silu(ctx_cond_ref[...].astype(F32).reshape(1, -1))
    cond_rows = jnp.where(pick == 0, cond_f, jnp.where(pick == 1, ctx_cond_f, 0.0)).astype(BF16)
    load_mod.wait()
    load_w = [
        load(2 + i, w, w_v.at[i])
        for i, w in enumerate((w_key_hbm, w_value_hbm, w_query_hbm, w_outgate_hbm))
    ]
    load_out = load(6, w_out_hbm, wout_v)
    part = jnp.dot(cond_rows, wm_v[...], preferred_element_type=F32)
    mod_part[sp] = part[:2]
    part_sent = spread("sp", sp, n, mod_part.at[sp], mod_part, part_send, part_recv)

    load_lat.wait()
    lat = lat_v[...].astype(F32)
    lat_r = lax.rsqrt(jnp.mean(lat * lat, axis=-1, keepdims=True) + norm_eps)
    collect("sp", sp, n, ctx_all, ctx_send, ctx_recv)
    ctx = ctx_all[...].astype(F32).reshape(ctx_len, depth)
    ctx_r = lax.rsqrt(jnp.mean(ctx * ctx, axis=-1, keepdims=True) + norm_eps)
    gain = gain_ref[...].astype(F32).reshape(1, depth)
    if rows > span + ctx_len:
        xin[span + ctx_len :, :] = jnp.zeros((rows - span - ctx_len, depth), BF16)
    ext_v[...] = jnp.zeros(ext_v.shape, F32)
    for d in range(2):
        ext_v[d * heads : (d + 1) * heads, :span] = extra_ref[0, d]

    collect("sp", sp, n, mod_part, part_send, part_recv)
    summed = mod_part[0]
    for j in range(1, n):
        summed = summed + mod_part[j]
    mod_full[tp] = summed
    full_sent = spread("tp", tp, t, mod_full.at[tp], mod_full, full_send, full_recv)

    at_row = lax.broadcasted_iota(jnp.int32, (rows, rows), 0)
    at_col = lax.broadcasted_iota(jnp.int32, (rows, rows), 1)
    same = (at_row < span) == (at_col < span)
    lane = lax.broadcasted_iota(jnp.int32, (1, rows), 1)
    is_lat = lane < span
    is_ctx = jnp.logical_and(lane >= span, lane < span + ctx_len)

    collect("tp", tp, t, mod_full, full_send, full_recv)
    modulation = jnp.concatenate([mod_full[j] for j in range(t)], axis=1)
    shift = modulation[:, :depth]
    scale = gain * (1.0 + modulation[:, depth : 2 * depth])
    gate = modulation[0:1, 2 * depth :]
    xin[:span, :] = (lat_v[...].astype(F32) * lat_r * scale[0:1] + shift[0:1]).astype(BF16)
    ctx = ctx_all[...].astype(F32).reshape(ctx_len, depth)
    xin[span : span + ctx_len, :] = (ctx * ctx_r * scale[1:2] + shift[1:2]).astype(BF16)

    wdb = jnp.concatenate(
        [w[d].astype(F32) for w in (w_decay_ref, w_beta_ref) for d in range(2)], axis=0
    ).astype(BF16)
    raw_t = lax.dot_general(
        wdb, xin[...], (((1,), (1,)), ((), ())), preferred_element_type=F32
    ).astype(BF16).astype(F32)

    def project(i):
        load_w[i].wait()
        return jnp.dot(xin[...], w_v[i], preferred_element_type=F32).astype(BF16).astype(F32)

    chain = lax.broadcasted_iota(jnp.int32, (chains, 1), 0)
    rate = jnp.zeros((chains, 1), F32)
    bias = jnp.zeros((chains, 1), F32)
    for c in range(chains):
        rate = jnp.where(chain == c, rate_ref[c // heads, c % heads], rate)
        bias = jnp.where(chain == c, bias_ref[c // heads, c % heads], bias)
    g = -rate * softplus(raw_t[:chains] + bias) + ext_v[:chains, :]
    g = jnp.where(jnp.logical_or(is_lat, is_ctx), g, 0.0)
    beta = beta_scale * rate / (1.0 + jnp.exp(-raw_t[chains : 2 * chains]))
    up_to = jnp.where(jnp.logical_and(same, at_row <= at_col), 1.0, 0.0)
    from_on = jnp.where(jnp.logical_and(same, at_row >= at_col), 1.0, 0.0)
    g_hi = g.astype(BF16).astype(F32)
    g_mid = (g - g_hi).astype(BF16).astype(F32)
    g_lo = g - g_hi - g_mid
    g_parts = jnp.concatenate([g_hi, g_mid, g_lo, jnp.zeros_like(g)], axis=0)
    sums_0 = mm(g_parts, up_to)
    sums_1 = mm(g_parts, from_on)

    def join(s):
        return s[:chains] + s[chains : 2 * chains] + s[2 * chains : 3 * chains]

    cum = jnp.where(chain < heads, join(sums_0), join(sums_1))
    tot_lat = jnp.sum(jnp.where(is_lat, g, 0.0), axis=-1, keepdims=True)
    tot_ctx = jnp.sum(jnp.where(is_ctx, g, 0.0), axis=-1, keepdims=True)
    to_end_lat = jnp.where(is_lat, jnp.exp(jnp.where(is_lat, tot_lat - cum, 0.0)), 0.0)
    to_end_ctx = jnp.where(is_ctx, jnp.exp(jnp.where(is_ctx, tot_ctx - cum, 0.0)), 0.0)
    through = jnp.exp(tot_lat)
    packed = jnp.concatenate(
        [cum, beta, jnp.zeros((HEAD - 2 * chains, rows), F32)], axis=0
    )
    cols = packed.T
    grow = jnp.exp(cols)

    key_raw, value_raw = project(0), project(1)
    keys, values, queries, keys_t = [], [], [], []
    for h in range(heads):
        part_h = slice(h * HEAD, (h + 1) * HEAD)
        k = unit_normal(silu(key_raw[:, part_h]))
        keys.append(k)
        keys_t.append(k.T)
        values.append(silu(value_raw[:, part_h]))
    kk = [mm_nt(k, k) for k in keys]

    tri = [at_row >= at_col, at_row <= at_col]
    weights, low, inv = [], [], []
    for c in range(chains):
        d, h = c // heads, c % heads
        mask = jnp.logical_and(same, tri[d])
        diff = cols[:, c : c + 1] - cum[c : c + 1, :]
        w = jnp.where(mask, jnp.exp(jnp.where(mask, diff, 0.0)), 0.0)
        weights.append(w)
        b = cols[:, chains + c : chains + c + 1]
        low.append(jnp.where(at_row != at_col, b * kk[h] * w, 0.0))
    half = 1
    while half < rows:
        pair = at_row // (2 * half) == at_col // (2 * half)
        cross = [
            jnp.logical_and(pair, jnp.logical_and(at_row // half % 2 == 1, at_col // half % 2 == 0)),
            jnp.logical_and(pair, jnp.logical_and(at_row // half % 2 == 0, at_col // half % 2 == 1)),
        ]
        coupling = [jnp.where(cross[c // heads], low[c], 0.0) for c in range(chains)]
        if half == 1:
            eye = jnp.where(at_row == at_col, 1.0, 0.0)
            inv = [eye - coupling[c] for c in range(chains)]
        else:
            inner_term = [mm(coupling[c], inv[c]) for c in range(chains)]
            inv = [inv[c] - mm(inv[c], inner_term[c]) for c in range(chains)]
        half *= 2

    eye_head = jnp.where(
        lax.broadcasted_iota(jnp.int32, (HEAD, HEAD), 0)
        == lax.broadcasted_iota(jnp.int32, (HEAD, HEAD), 1),
        1.0,
        0.0,
    )
    solved = []
    place = [sp, n - 1 - sp]
    for c in range(chains):
        d, h = c // heads, c % heads
        b = cols[:, chains + c : chains + c + 1]
        right = jnp.concatenate(
            [values[h] * b, keys[h] * (b * grow[:, c : c + 1])], axis=1
        )
        x = mm(inv[c], right)
        solved.append(x)
        ba = mm(keys_t[h] * to_end_lat[c : c + 1, :], x)
        ctx_state = mm(keys_t[h] * to_end_ctx[c : c + 1, :], x[:, :HEAD])
        a = eye_head * through[c : c + 1, :] - ba[:, HEAD:]
        b_map = ba[:, :HEAD]
        first = place[d] == 0
        own_a[c] = a
        own_b[c] = b_map
        pre_a[c] = jnp.where(first, 0.0, eye_head)
        pre_b[c] = jnp.where(first, ctx_state, 0.0)
        send_map[0, d, h] = jnp.where(first, 0.0, a).astype(BF16)
        send_map[0, d, heads + h] = (
            b_map + jnp.where(first, mm(a, ctx_state), 0.0)
        ).astype(BF16)

    def map_copy(level, d, k, which):
        part_of = pl.ds(which * heads, heads)
        target = lax.rem(sp + k, n) if d == 0 else lax.rem(sp + n - k, n)
        return pltpu.make_async_remote_copy(
            src_ref=send_map.at[level, d, part_of],
            dst_ref=recv_map.at[level, d, part_of],
            send_sem=map_send.at[level, d, which, k],
            recv_sem=map_recv.at[level, d, which],
            device_id={"sp": target},
            device_id_type=MESH,
        )

    def sends_map(level, d):
        wide = 1 << level
        at = place[d]
        return jnp.logical_and(lax.rem(at, 2 * wide) == wide - 1, at >= wide)

    def gets_map(level, d):
        wide = 1 << level
        at = place[d]
        return jnp.logical_and(lax.rem(at, 2 * wide) >= wide, at >= 2 * wide)

    levels = (n - 1).bit_length()

    def send_level(level):
        wide = 1 << level
        for d in range(2):

            @pl.when(lax.rem(place[d], 2 * wide) == wide - 1)
            def _():
                if level:
                    for h in range(heads):
                        c = d * heads + h
                        send_map[level, d, heads + h] = (
                            mm(own_a[c], pre_b[c]) + own_b[c]
                        ).astype(BF16)
                for k in range(wide, 0, -1):
                    map_copy(level, d, k, 1).start()

            if 2 * wide < n:

                @pl.when(sends_map(level, d))
                def _():
                    if level:
                        for h in range(heads):
                            c = d * heads + h
                            send_map[level, d, h] = mm(own_a[c], pre_a[c]).astype(BF16)
                    for k in range(wide, 0, -1):
                        map_copy(level, d, k, 0).start()

    def recv_level(level):
        wide = 1 << level
        for d in range(2):

            @pl.when(lax.rem(place[d], 2 * wide) >= wide)
            def _():
                map_copy(level, d, 1, 1).wait_recv()
                for h in range(heads):
                    c = d * heads + h
                    pre_b[c] = mm(pre_a[c], recv_map[level, d, heads + h]) + pre_b[c]

            if 2 * wide < n:

                @pl.when(gets_map(level, d))
                def _():
                    map_copy(level, d, 1, 0).wait_recv()
                    for h in range(heads):
                        c = d * heads + h
                        pre_a[c] = mm(pre_a[c], recv_map[level, d, h])

    if levels:
        send_level(0)

    query_raw, outgate_raw = project(2), project(3)
    local, mixers = [], []
    for h in range(heads):
        part_h = slice(h * HEAD, (h + 1) * HEAD)
        q = unit_normal(silu(query_raw[:, part_h])) * HEAD ** (-0.5)
        qk = mm_nt(q, keys[h])
        read = [mm(qk * weights[d * heads + h], solved[d * heads + h]) for d in range(2)]
        local.append(read[0][:, :HEAD] + read[1][:, :HEAD])
        mixers.append(
            jnp.concatenate(
                [
                    q * grow[:, d * heads + h : d * heads + h + 1] - read[d][:, HEAD:]
                    for d in range(2)
                ],
                axis=1,
            )
        )

    out_gate = [silu(outgate_raw[:, h * HEAD : (h + 1) * HEAD]) for h in range(heads)]
    for level in range(levels):
        recv_level(level)
        if level + 1 < levels:
            send_level(level + 1)

    out_gain = out_gain_ref[...].astype(F32)
    for h in range(heads):
        state = jnp.concatenate([pre_b[h], pre_b[heads + h]], axis=0)
        o = local[h] + mm(mixers[h], state)
        normed = o * lax.rsqrt(jnp.mean(o * o, axis=-1, keepdims=True) + norm_eps)
        gated = (normed * out_gain * out_gate[h]).astype(BF16)
        for j in range(t):
            gated_v[j, :, h * HEAD : (h + 1) * HEAD] = gated[j * rows_out : (j + 1) * rows_out]

    gate_sent = []
    for k in range(1, t):
        target = lax.rem(tp + k, t)
        copy = pltpu.make_async_remote_copy(
            src_ref=gated_v.at[target],
            dst_ref=gated_r.at[tp],
            send_sem=gate_send.at[k],
            recv_sem=gate_recv.at[k],
            device_id={"tp": target},
            device_id_type=MESH,
        )
        copy.start()
        gate_sent.append(copy)
    gated_r[tp] = gated_v[tp]
    load_out.wait()
    collect("tp", tp, t, gated_r, gate_send, gate_recv)
    by_rows = jnp.concatenate([gated_r[j] for j in range(t)], axis=1)
    mixed = jnp.dot(by_rows, wout_v[...], preferred_element_type=F32)
    own_rows = lat_v[pl.ds(pl.multiple_of(tp * rows_out, rows_out), rows_out), :].astype(F32)
    out_ref[0] = (own_rows + gate * mixed).astype(out_ref.dtype)

    for copy in ctx_sent + part_sent + full_sent + gate_sent:
        copy.wait_send()
    for level in range(levels):
        wide = 1 << level
        for d in range(2):

            @pl.when(lax.rem(place[d], 2 * wide) == wide - 1)
            def _():
                for k in range(1, wide + 1):
                    map_copy(level, d, k, 1).wait_send()

            if 2 * wide < n:

                @pl.when(sends_map(level, d))
                def _():
                    for k in range(1, wide + 1):
                        map_copy(level, d, k, 0).wait_send()


def on_device(
    n,
    t,
    latent,
    cond,
    context,
    ctx_cond,
    w_mod,
    norm_gain,
    w_query,
    w_key,
    w_value,
    w_outgate,
    w_decay,
    w_beta,
    decay_rate,
    decay_bias,
    extra_decay,
    out_gain,
    w_out,
):
    depth = latent.shape[2]
    span = latent.shape[1]
    heads = w_decay.shape[2]
    inner = heads * HEAD
    chains = 2 * heads
    ctx_len = n * context.shape[1]
    rows = -(-(span + ctx_len) // 128) * 128
    rows_out = span // t
    levels = max(1, (n - 1).bit_length())
    vmem = pl.BlockSpec(memory_space=pltpu.VMEM)
    smem = pl.BlockSpec(memory_space=pltpu.SMEM)
    hbm = pl.BlockSpec(memory_space=pl.ANY)
    dma = pltpu.SemaphoreType.DMA
    return pl.pallas_call(
        functools.partial(kernel, n, t, heads),
        out_shape=jax.ShapeDtypeStruct((1, rows_out, depth), BF16),
        in_specs=[smem] * 2 + [vmem] * 8 + [hbm] * 7,
        out_specs=vmem,
        scratch_shapes=[
            pltpu.VMEM((span, depth), BF16),
            pltpu.VMEM(w_mod.shape, BF16),
            pltpu.VMEM((4, depth, inner), BF16),
            pltpu.VMEM(w_out.shape, BF16),
            pltpu.VMEM((n,) + context.shape[1:], BF16),
            pltpu.VMEM((n, 2, w_mod.shape[1]), F32),
            pltpu.VMEM((t, 2, w_mod.shape[1]), F32),
            pltpu.VMEM((rows, depth), BF16),
            pltpu.VMEM((8, rows), F32),
            pltpu.VMEM((chains, HEAD, HEAD), F32),
            pltpu.VMEM((chains, HEAD, HEAD), F32),
            pltpu.VMEM((chains, HEAD, HEAD), F32),
            pltpu.VMEM((chains, HEAD, HEAD), F32),
            pltpu.VMEM((levels, 2, 2 * heads, HEAD, HEAD), BF16),
            pltpu.VMEM((levels, 2, 2 * heads, HEAD, HEAD), BF16),
            pltpu.VMEM((t, rows_out, inner), BF16),
            pltpu.VMEM((t, rows_out, inner), BF16),
            dma((7,)),
            dma((n,)),
            dma((n,)),
            dma((n,)),
            dma((n,)),
            dma((t,)),
            dma((t,)),
            dma((levels, 2, 2, n)),
            dma((levels, 2, 2)),
            dma((t,)),
            dma((t,)),
        ],
        compiler_params=pltpu.CompilerParams(
            collective_id=0, has_side_effects=True, vmem_limit_bytes=60 * 1024 * 1024
        ),
    )(
        decay_rate,
        decay_bias,
        cond,
        ctx_cond,
        context,
        norm_gain,
        out_gain[None, :],
        jnp.transpose(w_decay, (1, 2, 0)),
        jnp.transpose(w_beta, (1, 2, 0)),
        extra_decay,
        latent,
        w_mod,
        w_query,
        w_outgate,
        w_key,
        w_value,
        w_out,
    )


def solution(mesh):
    placed = (
        P("dp", "sp", None),
        P("dp", "sp"),
        P("dp", "sp", None),
        P("sp"),
        P("sp", "tp"),
        P(),
        P(None, "tp"),
        P(None, "tp"),
        P(None, "tp"),
        P(None, "tp"),
        P(None, None, "tp"),
        P(None, None, "tp"),
        P(None, "tp"),
        P(None, "tp"),
        P("dp", None, "tp", "sp"),
        P(),
        P(),
    )
    return jax.shard_map(
        functools.partial(on_device, mesh.shape["sp"], mesh.shape["tp"]),
        mesh=mesh,
        in_specs=placed,
        out_specs=P("dp", ("sp", "tp"), None),
        check_vma=False,
    )
```
